32 devices in a mesh: fs: 8 (over z, y), tp: 4 (over x, core).
Axes of the slice: x: 2, y: 2, z: 4, core: 2. Of those that a mesh axis runs over, the one named last changes fastest.
Arguments:
- inputs: bfloat16 [4096, 2048], P(('fs', 'tp')), may hold values from -6 to 6
- w_gate: float32 [2048, 5632], P('fs', 'tp'), may hold values from -0.125 to 0.125
- w_value: float32 [2048, 5632], P('fs', 'tp'), may hold values from -0.125 to 0.125
- gate_scale: float32 [5632], P('tp'), may hold values from 0.5 to 2
- value_scale: float32 [5632], P('tp'), may hold values from 0.5 to 2
- conv_gate: float32 [3, 5632], P(None, 'tp'), may hold values from -3.5 to 3.5
- conv_value: float32 [3, 5632], P(None, 'tp'), may hold values from -3.5 to 3.5
- gate_pre: bfloat16 [4096, 5632], P('fs', 'tp'), may hold values from -6 to 6
- value_pre: bfloat16 [4096, 5632], P('fs', 'tp'), may hold values from -6 to 6
- grad_out: bfloat16 [4096, 5632], P('fs', 'tp'), may hold values from -6 to 6
Outputs:
- grad_inputs: bfloat16 [4096, 2048], P(('fs', 'tp'))
- grad_w_gate: float32 [2048, 5632], P('fs', 'tp')
- grad_w_value: float32 [2048, 5632], P('fs', 'tp')
- grad_gate_scale: float32 [5632], P('tp')
- grad_value_scale: float32 [5632], P('tp')
- grad_conv_gate: float32 [3, 5632], P(None, 'tp')
- grad_conv_value: float32 [3, 5632], P(None, 'tp')
The draws below stay inside these ranges and needn't reach their ends.
All inputs are finite; a program needn't handle non-finite values.
Results may differ from the reference program's by a relative error of at most 0.015.
Values may be sent and summed in bfloat16 or wider, within the bound.
No kernel may reach another device: no remote copies, remote signals or barrier semaphores. Data moves between devices by JAX's collectives and lax.ppermute only.
A program may use at most 128 MiB of HBM per device.

```python
import math
import jax
import jax.numpy as jnp

D = 2048
FF = 5632
KW = 3
SEQ = 512
TOKENS = 4096
N_FS = 8
N_TP = 4


def strengthened(result, rng, source, target, parts, factor):
    def block_of(position):
        return (jnp.arange(result.shape[position]) // (result.shape[position] // parts)).reshape((-1,) + (1,) * (result.ndim - 1 - position))

    one_side = jax.random.permutation(rng, parts)[block_of(target)]
    second = (block_of(target) + parts // 2) % parts
    return jnp.where((block_of(source) == one_side) | (block_of(source) == second), factor * result, result)


def levels(key, dims, split, least, largest):
    factor_of = 1.0
    for dim, shards_of in split:
        draws = jax.random.uniform(jax.random.fold_in(jax.random.fold_in(key, 6), dim), (shards_of,), jnp.float32, least / len(split), largest / len(split))
        factor_of = factor_of * jnp.repeat(jnp.exp(draws), dims[dim] // shards_of).reshape((-1,) + (1,) * (len(dims) - 1 - dim))
    return factor_of


def bell_draw(rng, dims, scale, most, shards=(), held_as=jnp.bfloat16):
    result = jax.random.normal(rng, dims, jnp.float32) * scale
    if len(shards) > 0:
        result = levels(rng, dims, shards, -0.22, 0.18) * result
    return jnp.clip(result, min=-most, max=most).astype(held_as)


def gaussian_with(stream_key, extent, spread, reach, shards, heavy, dtype=jnp.bfloat16):
    array = spread * jax.random.normal(stream_key, extent, jnp.float32)
    if shards:
        array = array * levels(stream_key, extent, shards, -0.22, 0.18)
    return jnp.clip(strengthened(array, jax.random.fold_in(stream_key, 3), *heavy), -reach, reach).astype(dtype)


def setup_inputs(seed: int = 0) -> dict:
    key_of = jax.random.split(jax.random.key(seed), 11)
    inputs = gaussian_with(key_of[0], (TOKENS, D), 1.0, 6.0, ((0, 32),), (0, 1, 32, 2.75))
    w_gate = bell_draw(key_of[1], (D, FF), D ** -0.5, 0.125, ((0, 8), (1, 4)), jnp.float32)
    w_value = bell_draw(key_of[2], (D, FF), D ** -0.5, 0.125, ((0, 8), (1, 4)), jnp.float32)
    gate_scale = jnp.clip(jnp.exp(math.log(2.0) - 1.3862944 * jax.random.uniform(key_of[3], (FF,), jnp.float32) ** levels(key_of[3], (FF,), ((0, 4),), -0.2, 0.2)), 0.5, 2.0)
    value_scale = jnp.clip(jnp.exp(math.log(2.0) - 1.3862944 * jax.random.uniform(key_of[4], (FF,), jnp.float32) ** levels(key_of[4], (FF,), ((0, 4),), -0.2, 0.2)), 0.5, 2.0)
    conv_gate = bell_draw(key_of[5], (KW, FF), KW ** -0.5, 3.5, ((1, 4),), jnp.float32)
    conv_value = bell_draw(key_of[6], (KW, FF), KW ** -0.5, 3.5, ((1, 4),), jnp.float32)
    gate_pre = bell_draw(key_of[7], (TOKENS, FF), 1.0, 6.0, ((0, 8), (1, 4)))
    value_pre = bell_draw(key_of[8], (TOKENS, FF), 1.0, 6.0, ((0, 8), (1, 4)))
    grad_out = gaussian_with(key_of[9], (TOKENS, FF), 1.0, 6.0, ((0, 8), (1, 4)), (0, 1, 8, 2.0))
    return {"inputs": inputs, "w_gate": w_gate, "w_value": w_value, "gate_scale": gate_scale, "value_scale": value_scale, "conv_gate": conv_gate, "conv_value": conv_value, "gate_pre": gate_pre, "value_pre": value_pre, "grad_out": grad_out}


def shift_down(field, steps):
    return jnp.pad(field, ((0, 0), (steps, 0), (0, 0)))[:, :field.shape[1]]


def shift_up(field, steps):
    return jnp.pad(field, ((0, 0), (0, steps), (0, 0)))[:, steps:]


def reference(inputs, w_gate, w_value, gate_scale, value_scale, conv_gate, conv_value, gate_pre, value_pre, grad_out):
    gate_raw = gate_pre.astype(jnp.float32).reshape(N_FS, SEQ, FF)
    value_raw = value_pre.astype(jnp.float32).reshape(N_FS, SEQ, FF)
    gate_lin = gate_raw * gate_scale
    value_lin = value_raw * value_scale
    gate_conv = conv_gate[2] * gate_lin + conv_gate[1] * shift_down(gate_lin, 1) + conv_gate[0] * shift_down(gate_lin, 2)
    value_conv = conv_value[2] * value_lin + conv_value[1] * shift_down(value_lin, 1) + conv_value[0] * shift_down(value_lin, 2)
    sig = jax.nn.sigmoid(gate_conv)
    upstream = grad_out.astype(jnp.float32).reshape(N_FS, SEQ, FF)
    d_gate_conv = upstream * value_conv * sig * (1.0 + gate_conv * (1.0 - sig))
    d_value_conv = upstream * gate_conv * sig
    grad_conv_gate = jnp.stack([jnp.sum(d_gate_conv * shift_down(gate_lin, 2), axis=(0, 1)),
                                jnp.sum(d_gate_conv * shift_down(gate_lin, 1), axis=(0, 1)),
                                jnp.sum(d_gate_conv * gate_lin, axis=(0, 1))])
    grad_conv_value = jnp.stack([jnp.sum(d_value_conv * shift_down(value_lin, 2), axis=(0, 1)),
                                 jnp.sum(d_value_conv * shift_down(value_lin, 1), axis=(0, 1)),
                                 jnp.sum(d_value_conv * value_lin, axis=(0, 1))])
    d_gate_lin = conv_gate[2] * d_gate_conv + conv_gate[1] * shift_up(d_gate_conv, 1) + conv_gate[0] * shift_up(d_gate_conv, 2)
    d_value_lin = conv_value[2] * d_value_conv + conv_value[1] * shift_up(d_value_conv, 1) + conv_value[0] * shift_up(d_value_conv, 2)
    grad_gate_scale = jnp.sum(d_gate_lin * gate_raw, axis=(0, 1))
    grad_value_scale = jnp.sum(d_value_lin * value_raw, axis=(0, 1))
    d_gate_lin = d_gate_lin.reshape(TOKENS, FF)
    d_value_lin = d_value_lin.reshape(TOKENS, FF)
    gate_cot = d_gate_lin.astype(jnp.bfloat16)
    value_cot = d_value_lin.astype(jnp.bfloat16)
    gate_back = (d_gate_lin * gate_scale).astype(jnp.bfloat16)
    value_back = (d_value_lin * value_scale).astype(jnp.bfloat16)
    grad_w_gate = jnp.dot(inputs.T, gate_cot, preferred_element_type=jnp.float32) * gate_scale
    grad_w_value = jnp.dot(inputs.T, value_cot, preferred_element_type=jnp.float32) * value_scale
    gate_half = w_gate.astype(jnp.bfloat16)
    value_half = w_value.astype(jnp.bfloat16)
    width = FF // N_TP
    total = jnp.zeros((TOKENS, D), jnp.float32)
    for block in range(N_TP):
        lo = block * width
        part = jnp.dot(gate_back[:, lo:lo + width], gate_half[:, lo:lo + width].T, preferred_element_type=jnp.float32)
        part = part + jnp.dot(value_back[:, lo:lo + width], value_half[:, lo:lo + width].T, preferred_element_type=jnp.float32)
        total = total + part.astype(jnp.bfloat16).astype(jnp.float32)
    grad_inputs = total.astype(jnp.bfloat16)
    return (grad_inputs, grad_w_gate, grad_w_value, grad_gate_scale, grad_value_scale, grad_conv_gate, grad_conv_value)
```

```python
import jax
import jax.numpy as jnp
from jax import lax
from jax.sharding import PartitionSpec as P


def shift_down(field, steps):
    return jnp.pad(field, ((steps, 0), (0, 0)))[: field.shape[0]]


def shift_up(field, steps):
    return jnp.pad(field, ((0, steps), (0, 0)))[steps:]


def on_device(
    inputs,
    w_gate,
    w_value,
    gate_scale,
    value_scale,
    conv_gate,
    conv_value,
    gate_pre,
    value_pre,
    grad_out,
):
    gate_raw = gate_pre.astype(jnp.float32)
    value_raw = value_pre.astype(jnp.float32)
    gate_lin = gate_raw * gate_scale
    value_lin = value_raw * value_scale
    gate_conv = (
        conv_gate[2] * gate_lin
        + conv_gate[1] * shift_down(gate_lin, 1)
        + conv_gate[0] * shift_down(gate_lin, 2)
    )
    value_conv = (
        conv_value[2] * value_lin
        + conv_value[1] * shift_down(value_lin, 1)
        + conv_value[0] * shift_down(value_lin, 2)
    )
    sig = jax.nn.sigmoid(gate_conv)
    upstream = grad_out.astype(jnp.float32)
    d_gate_conv = upstream * value_conv * sig * (1.0 + gate_conv * (1.0 - sig))
    d_value_conv = upstream * gate_conv * sig
    taps_gate = jnp.stack(
        [
            jnp.sum(d_gate_conv * shift_down(gate_lin, 2), axis=0),
            jnp.sum(d_gate_conv * shift_down(gate_lin, 1), axis=0),
            jnp.sum(d_gate_conv * gate_lin, axis=0),
        ]
    )
    taps_value = jnp.stack(
        [
            jnp.sum(d_value_conv * shift_down(value_lin, 2), axis=0),
            jnp.sum(d_value_conv * shift_down(value_lin, 1), axis=0),
            jnp.sum(d_value_conv * value_lin, axis=0),
        ]
    )
    d_gate_lin = (
        conv_gate[2] * d_gate_conv
        + conv_gate[1] * shift_up(d_gate_conv, 1)
        + conv_gate[0] * shift_up(d_gate_conv, 2)
    )
    d_value_lin = (
        conv_value[2] * d_value_conv
        + conv_value[1] * shift_up(d_value_conv, 1)
        + conv_value[0] * shift_up(d_value_conv, 2)
    )
    scale_gate = jnp.sum(d_gate_lin * gate_raw, axis=0)
    scale_value = jnp.sum(d_value_lin * value_raw, axis=0)
    sums = lax.psum((scale_gate, scale_value, taps_gate, taps_value), "fs")
    gate_cot = d_gate_lin.astype(jnp.bfloat16)
    value_cot = d_value_lin.astype(jnp.bfloat16)
    n_fs = lax.axis_size("fs")
    n_tp = lax.axis_size("tp")
    swap = [(i, i ^ 1) for i in range(n_fs)]
    groups = [list(range(p, n_fs, 2)) for p in range(2)]
    parity = lax.axis_index("fs") % 2
    me = lax.axis_index("tp")
    rows = w_gate.shape[0]
    half = rows * n_fs // 2
    own_tokens = inputs.shape[0]

    split = inputs.reshape(own_tokens, n_fs // 2, 2, rows)
    keep = lax.dynamic_index_in_dim(split, parity, 2, False).reshape(own_tokens, half)
    give = lax.dynamic_index_in_dim(split, 1 - parity, 2, False).reshape(own_tokens, half)
    got = lax.ppermute(give, "fs", swap)
    tokens = lax.all_gather(jnp.stack([keep, got]), "tp", axis=1, tiled=True)

    scaled = jnp.concatenate(
        [
            (w_gate * gate_scale).astype(jnp.bfloat16),
            (w_value * value_scale).astype(jnp.bfloat16),
        ],
        axis=1,
    )
    weights = lax.all_gather(scaled, "fs", axis=0, tiled=True, axis_index_groups=groups)

    columns = gate_cot.shape[1]
    gate_other = lax.ppermute(gate_cot, "fs", swap)
    value_other = lax.ppermute(value_cot, "fs", swap)

    def outer(left, right):
        return lax.dot_general(
            left, right, (((0,), (0,)), ((), ())), preferred_element_type=jnp.float32
        )

    def weight_grad(own, other, scale):
        total = outer(tokens[0], own) + outer(tokens[1], other)
        summed = lax.psum_scatter(
            total.astype(jnp.bfloat16), "fs", scatter_dimension=0, tiled=True,
            axis_index_groups=groups,
        )
        return summed.astype(jnp.float32) * scale

    grad_w_gate = weight_grad(gate_cot, gate_other, gate_scale)
    grad_w_value = weight_grad(value_cot, value_other, value_scale)

    def inner(gate_side, value_side):
        dims = (((1,), (1,)), ((), ()))
        return (
            lax.dot_general(
                gate_side, weights[:, :columns], dims, preferred_element_type=jnp.float32
            )
            + lax.dot_general(
                value_side, weights[:, columns:], dims, preferred_element_type=jnp.float32
            )
        ).astype(jnp.bfloat16)

    def reduce_tp(part):
        blocks = part.reshape(n_tp, own_tokens, half)
        total = lax.dynamic_index_in_dim(blocks, me, 0, False).astype(jnp.float32)
        for shift in range(1, n_tp):
            block = lax.dynamic_index_in_dim(blocks, (me + shift) % n_tp, 0, False)
            ring = [(i, (i + shift) % n_tp) for i in range(n_tp)]
            total = total + lax.ppermute(block, "tp", ring).astype(jnp.float32)
        return total.astype(jnp.bfloat16)

    mine = reduce_tp(inner(gate_cot, value_cot))
    theirs = reduce_tp(inner(gate_other, value_other))
    returned = lax.ppermute(theirs, "fs", swap)
    even = jnp.where(parity == 0, mine, returned).reshape(own_tokens, n_fs // 2, 1, rows)
    odd = jnp.where(parity == 0, returned, mine).reshape(own_tokens, n_fs // 2, 1, rows)
    grad_inputs = jnp.concatenate([even, odd], axis=2).reshape(own_tokens, half * 2)
    return (grad_inputs, grad_w_gate, grad_w_value, sums[0], sums[1], sums[2], sums[3])


def solution(mesh):
    placed = (
        P(("fs", "tp"), None),
        P("fs", "tp"),
        P("fs", "tp"),
        P("tp"),
        P("tp"),
        P(None, "tp"),
        P(None, "tp"),
        P("fs", "tp"),
        P("fs", "tp"),
        P("fs", "tp"),
    )
    return jax.shard_map(
        on_device,
        mesh=mesh,
        in_specs=placed,
        out_specs=(
            P(("fs", "tp"), None),
            P("fs", "tp"),
            P("fs", "tp"),
            P("tp"),
            P("tp"),
            P(None, "tp"),
            P(None, "tp"),
        ),
        check_vma=False,
    )
```

```python
import jax
import jax.numpy as jnp
from jax import lax
from jax.sharding import PartitionSpec as P


def shift_down(field, steps):
    return jnp.pad(field, ((steps, 0), (0, 0)))[: field.shape[0]]


def shift_up(field, steps):
    return jnp.pad(field, ((0, steps), (0, 0)))[steps:]


def on_device(
    inputs,
    w_gate,
    w_value,
    gate_scale,
    value_scale,
    conv_gate,
    conv_value,
    gate_pre,
    value_pre,
    grad_out,
):
    gate_raw = gate_pre.astype(jnp.float32)
    value_raw = value_pre.astype(jnp.float32)
    gate_lin = gate_raw * gate_scale
    value_lin = value_raw * value_scale
    gate_conv = (
        conv_gate[2] * gate_lin
        + conv_gate[1] * shift_down(gate_lin, 1)
        + conv_gate[0] * shift_down(gate_lin, 2)
    )
    value_conv = (
        conv_value[2] * value_lin
        + conv_value[1] * shift_down(value_lin, 1)
        + conv_value[0] * shift_down(value_lin, 2)
    )
    sig = jax.nn.sigmoid(gate_conv)
    upstream = grad_out.astype(jnp.float32)
    d_gate_conv = upstream * value_conv * sig * (1.0 + gate_conv * (1.0 - sig))
    d_value_conv = upstream * gate_conv * sig
    taps_gate = jnp.stack(
        [
            jnp.sum(d_gate_conv * shift_down(gate_lin, 2), axis=0),
            jnp.sum(d_gate_conv * shift_down(gate_lin, 1), axis=0),
            jnp.sum(d_gate_conv * gate_lin, axis=0),
        ]
    )
    taps_value = jnp.stack(
        [
            jnp.sum(d_value_conv * shift_down(value_lin, 2), axis=0),
            jnp.sum(d_value_conv * shift_down(value_lin, 1), axis=0),
            jnp.sum(d_value_conv * value_lin, axis=0),
        ]
    )
    d_gate_lin = (
        conv_gate[2] * d_gate_conv
        + conv_gate[1] * shift_up(d_gate_conv, 1)
        + conv_gate[0] * shift_up(d_gate_conv, 2)
    )
    d_value_lin = (
        conv_value[2] * d_value_conv
        + conv_value[1] * shift_up(d_value_conv, 1)
        + conv_value[0] * shift_up(d_value_conv, 2)
    )
    scale_gate = jnp.sum(d_gate_lin * gate_raw, axis=0)
    scale_value = jnp.sum(d_value_lin * value_raw, axis=0)
    sums = jnp.concatenate([scale_gate[None], scale_value[None], taps_gate, taps_value], axis=0)
    width = lax.axis_size("fs")
    if width & (width - 1):
        sums = lax.psum(sums, "fs")
    else:
        step = 1
        while step < width:
            sums = sums + lax.ppermute(sums, "fs", [(i, i ^ step) for i in range(width)])
            step *= 2
    gate_cot = d_gate_lin.astype(jnp.bfloat16)
    value_cot = d_value_lin.astype(jnp.bfloat16)
    n_fs = lax.axis_size("fs")
    n_tp = lax.axis_size("tp")
    swap = [(i, i ^ 1) for i in range(n_fs)]
    groups = [list(range(p, n_fs, 2)) for p in range(2)]
    ring_size = n_fs // 2
    place = lax.axis_index("fs") // 2
    up = [(i, (i + 2) % n_fs) for i in range(n_fs)]
    down = [(i, (i - 2) % n_fs) for i in range(n_fs)]
    parity = lax.axis_index("fs") % 2
    me = lax.axis_index("tp")
    rows = w_gate.shape[0]
    half = rows * n_fs // 2
    own_tokens = inputs.shape[0]

    split = inputs.reshape(own_tokens, n_fs // 2, 2, rows)
    keep = lax.dynamic_index_in_dim(split, parity, 2, False).reshape(own_tokens, half)
    give = lax.dynamic_index_in_dim(split, 1 - parity, 2, False).reshape(own_tokens, half)
    got = lax.ppermute(give, "fs", swap)
    tokens = lax.all_gather(jnp.stack([keep, got]), "tp", axis=1, tiled=True)

    scaled = jnp.concatenate(
        [
            (w_gate * gate_scale).astype(jnp.bfloat16),
            (w_value * value_scale).astype(jnp.bfloat16),
        ],
        axis=1,
    )
    columns = gate_cot.shape[1]
    gate_other = lax.ppermute(gate_cot, "fs", swap)
    value_other = lax.ppermute(value_cot, "fs", swap)
    pieces = [scaled] + [None] * (ring_size - 1)
    rising = falling = scaled
    for hop in range(1, ring_size // 2 + 1):
        if 2 * hop == ring_size:
            pieces[hop] = jnp.concatenate(
                [
                    lax.ppermute(rising[:, :columns], "fs", up),
                    lax.ppermute(falling[:, columns:], "fs", down),
                ],
                axis=1,
            )
        else:
            rising = lax.ppermute(rising, "fs", up)
            falling = lax.ppermute(falling, "fs", down)
            if hop == 1:
                gate_other, rising, falling = lax.optimization_barrier(
                    (gate_other, rising, falling)
                )
            pieces[hop] = rising
            pieces[ring_size - hop] = falling
    value_other, pieces = lax.optimization_barrier((value_other, pieces))
    weights = jnp.concatenate(pieces, axis=0)


    def outer(left, right):
        return lax.dot_general(
            left, right, (((0,), (0,)), ((), ())), preferred_element_type=jnp.float32
        )

    def weight_grad(own, other):
        return (outer(tokens[0], own) + outer(tokens[1], other)).astype(jnp.bfloat16)

    def ring_scatter(blocks, route, sign):
        def block(at):
            return lax.dynamic_index_in_dim(blocks, at % ring_size, 0, False)

        total = block(place - sign + ring_size)
        for hop in range(1, ring_size):
            moved = lax.ppermute(total.astype(jnp.bfloat16), "fs", route)
            total = moved.astype(jnp.float32) + block(
                place - sign * (1 + hop) + 2 * ring_size
            ).astype(jnp.float32)
        return total.astype(jnp.float32)

    gate_total = weight_grad(gate_cot, gate_other)
    value_total = weight_grad(value_cot, value_other).reshape(ring_size, rows, columns)
    gate_sum = lax.psum_scatter(
        gate_total, "fs", scatter_dimension=0, tiled=True, axis_index_groups=groups
    )
    middle = (columns // 256) * 128
    value_sum = jnp.concatenate(
        [
            ring_scatter(value_total[:, :, :middle], up, 1),
            ring_scatter(value_total[:, :, middle:], down, -1),
        ],
        axis=1,
    )
    grad_w_gate = gate_sum.astype(jnp.float32) * gate_scale
    grad_w_value = value_sum * value_scale

    def inner(gate_side, value_side):
        dims = (((1,), (1,)), ((), ()))
        return (
            lax.dot_general(
                gate_side, weights[:, :columns], dims, preferred_element_type=jnp.float32
            )
            + lax.dot_general(
                value_side, weights[:, columns:], dims, preferred_element_type=jnp.float32
            )
        ).astype(jnp.bfloat16)

    def reduce_tp(part):
        blocks = part.reshape(n_tp, own_tokens, half)
        total = lax.dynamic_index_in_dim(blocks, me, 0, False).astype(jnp.float32)
        for shift in range(1, n_tp):
            block = lax.dynamic_index_in_dim(blocks, (me + shift) % n_tp, 0, False)
            ring = [(i, (i + shift) % n_tp) for i in range(n_tp)]
            total = total + lax.ppermute(block, "tp", ring).astype(jnp.float32)
        return total.astype(jnp.bfloat16)

    mine = reduce_tp(inner(gate_cot, value_cot))
    theirs = reduce_tp(inner(gate_other, value_other))
    returned = lax.ppermute(theirs, "fs", swap)
    even = jnp.where(parity == 0, mine, returned).reshape(own_tokens, ring_size, rows)
    odd = jnp.where(parity == 0, returned, mine).reshape(own_tokens, ring_size, rows)
    parts = []
    for at in range(ring_size):
        index = (place - at + ring_size) % ring_size
        parts.append(lax.dynamic_index_in_dim(even, index, 1, False))
        parts.append(lax.dynamic_index_in_dim(odd, index, 1, False))
    grad_inputs = jnp.concatenate(parts, axis=1)
    return (grad_inputs, grad_w_gate, grad_w_value, sums[0], sums[1], sums[2:5], sums[5:])


def solution(mesh):
    placed = (
        P(("fs", "tp"), None),
        P("fs", "tp"),
        P("fs", "tp"),
        P("tp"),
        P("tp"),
        P(None, "tp"),
        P(None, "tp"),
        P("fs", "tp"),
        P("fs", "tp"),
        P("fs", "tp"),
    )
    return jax.shard_map(
        on_device,
        mesh=mesh,
        in_specs=placed,
        out_specs=(
            P(("fs", "tp"), None),
            P("fs", "tp"),
            P("fs", "tp"),
            P("tp"),
            P("tp"),
            P(None, "tp"),
            P(None, "tp"),
        ),
        check_vma=False,
    )
```
